32 devices in a mesh: sp: 8 (over z, x), tp: 4 (over y, core).
Axes of the slice: x: 2, y: 2, z: 4, core: 2. Of those that a mesh axis runs over, the one named last changes fastest.
Arguments:
- moe_input: bfloat16 [2048, 2048], P('sp'), may hold values from -6 to 6
- out_cotangent: bfloat16 [2048, 2048], P('sp'), may hold values from -6 to 6
- routes: int32 [2048, 2], P('sp'), may hold values from 0 to 7, all different within a row; in each aligned block of 256 rows (0 to 255, 256 to 511, ...) at most 96 rows name the same one
- group_weight: float32 [2048], P('sp'), may hold values from 0.5 to 1
- inner_weight: float32 [2048, 2], P('sp'), may hold values from 0.3 to 1
- gate_weight: bfloat16 [8, 2048, 1024], P('sp', None, 'tp'), may hold values from -0.125 to 0.125
- up_weight: bfloat16 [8, 2048, 1024], P('sp', None, 'tp'), may hold values from -0.125 to 0.125
- down_weight: bfloat16 [8, 1024, 2048], P('sp', 'tp'), may hold values from -0.1875 to 0.1875
- value_in: bfloat16 [2048, 1024], P('sp', 'tp'), may hold values from -6 to 6
- gate_in: bfloat16 [2048, 1024], P('sp', 'tp'), may hold values from -6 to 6
- conv_taps: bfloat16 [31, 1024], P(None, 'tp'), may hold values from -1 to 1
- norm_hat: bfloat16 [2048, 1024], P('sp', 'tp'), may hold values from -6 to 6
- norm_rstd: float32 [2048], P('sp'), may hold values from 0.3 to 3
- norm_gain: float32 [1024], P('tp'), may hold values from 0.1 to 1.9
- out_proj: bfloat16 [2048, 1024], P(None, 'tp'), may hold values from -0.1875 to 0.1875
Outputs:
- gate_grad: bfloat16 [8, 2048, 1024], P('sp', None, 'tp')
- up_grad: bfloat16 [8, 2048, 1024], P('sp', None, 'tp')
- down_grad: bfloat16 [8, 1024, 2048], P('sp', 'tp')
- proj_grad: float32 [2048, 1024], P('sp', 'tp')
- value_grad: bfloat16 [2048, 1024], P('sp', 'tp')
- gate_in_grad: bfloat16 [2048, 1024], P('sp', 'tp')
The draws below stay inside these ranges and needn't reach their ends.
Inputs may be any that keep to these rules, and one draw needn't show every extreme that they name: In the rows of one device (aligned blocks of 256 tokens) no expert is named by more than 96 routes, and in every draw some expert is named by exactly 96 in some block; a token's two experts differ.
All inputs are finite; a program needn't handle non-finite values.
Results may differ from the reference program's by a relative error of at most 0.009.
Values may be sent and summed in bfloat16 or wider, within the bound.
No kernel may reach another device: no remote copies, remote signals or barrier semaphores. Data moves between devices by JAX's collectives and lax.ppermute only.
A program may use at most 128 MiB of HBM per device.

```python
import math
import jax
import jax.numpy as jnp
import numpy as np
from jax import lax

D = 2048
CONV = 1024
FF = 1024
KERNEL = 31
TOK_DEV = 256
EXPERTS = 8
CAP = 96
TOKENS = 2048
N_TP = 4


def raised(array, own_key, source, target, blocks, factor):
    owner, partner = [(jnp.arange(array.shape[axis_at]) // (array.shape[axis_at] // blocks)).reshape([-1 if axis == axis_at else 1 for axis in range(array.ndim)]) for axis_at in (source, target)]
    chosen = jax.random.permutation(own_key, blocks)[partner]
    strong = (owner == chosen) | (owner == (partner + blocks // 2) % blocks)
    return jnp.where(strong, factor * array, array)


def steps_of(own_key, extent, split, smallest, largest):
    level = 1.0
    for axis_at, shards_of in split:
        steps = jax.random.uniform(jax.random.fold_in(jax.random.fold_in(own_key, 6), axis_at), (shards_of,), jnp.float32, smallest / len(split), largest / len(split))
        level = level * jnp.repeat(jnp.exp(steps), extent[axis_at] // shards_of).reshape((-1,) + (1,) * (len(extent) - 1 - axis_at))
    return level


def deal_out(key, own, number, rows, number_of, top, most, lean):
    sequence = jax.random.permutation(key, number_of)
    crowded, common = shares(number_of, rows * top, most, lean, True), shares(number_of, rows * top, most, lean, False)
    places = jnp.arange(number_of)

    def named(sizes, rotation):
        used = int((sizes > 0).sum())
        fixed = max(1, used // 4)
        passed = fixed + (places - fixed + rotation * (used - fixed)) % max(1, number_of - fixed)
        return jnp.zeros((number_of,), jnp.int32).at[sequence[jnp.where(places < fixed, places, passed)]].set(jnp.asarray(sizes, jnp.int32))

    sizes = jnp.where(number % 4 == 0, named(crowded, number // 4), named(common, number - number // 4 - 1))
    mixed = jax.random.permutation(jax.random.fold_in(own, 3), number_of)
    source_of, sink = mixed[0:number_of // 2 * 2:2], mixed[1:number_of // 2 * 2:2]
    room = jnp.minimum(sizes[source_of] - 1, most - sizes[sink]) // 2
    room = jnp.where((source_of == sequence[0]) | (sink == sequence[0]) | (sizes[sink] == 0), 0, jnp.maximum(room, 0))
    passed = jax.random.randint(jax.random.fold_in(own, 4), (number_of // 2,), 0, 1 << 20) % (room + 1)
    sizes = sizes.at[source_of].add(-passed).at[sink].add(passed)
    items = jnp.searchsorted(jnp.cumsum(sizes), jnp.arange(rows * top), side="right").astype(jnp.int32)
    grid = items.reshape(top, rows).T
    grid = grid[jax.random.permutation(jax.random.fold_in(own, 1), rows)]
    rotation = jax.random.randint(jax.random.fold_in(own, 2), (rows, 1), 0, top)
    return jnp.take_along_axis(grid, (jnp.arange(top)[None, :] + rotation) % top, axis=1)


def shares(number_of, total, limit, slope, full):
    weights = [(1 << 20) // math.isqrt(grade ** slope) + 1 for grade in range(1, number_of + 1)]
    largest = limit if full else min(limit, max(-(-total // number_of), total * weights[0] // sum(weights)))
    least = 1 if total - largest >= number_of - 1 else 0
    counts, surplus = [largest] + [least] * (number_of - 1), total - largest - least * (number_of - 1)
    while surplus > 0:
        candidates = [i for i in range(1, number_of) if counts[i] < largest] or [i for i in range(1, number_of) if counts[i] < limit]
        pool, left = sum([weights[i] for i in candidates]), surplus
        for i in candidates:
            extra = min(limit - counts[i], max(1, left * weights[i] // pool), surplus)
            counts[i] = counts[i] + extra
            surplus = surplus - extra
    return np.array(counts)


def noise(stream_key, dims, spread, limit, split=(), kind=jnp.bfloat16):
    values = spread * jax.random.normal(stream_key, dims, jnp.float32)
    if split:
        values = values * steps_of(stream_key, dims, split, -0.22, 0.18)
    return jnp.clip(values, -limit, limit).astype(kind)


def gaussian_with(rng, dims, deviation, limit, shards, heavy, kind=jnp.bfloat16):
    drawn = deviation * jax.random.normal(rng, dims, jnp.float32)
    if shards:
        drawn = drawn * steps_of(rng, dims, shards, -0.22, 0.18)
    return jnp.clip(raised(drawn, jax.random.fold_in(rng, 3), *heavy), -limit, limit).astype(kind)


def setup_inputs(seed: int = 0) -> dict:
    seeds = jax.random.split(jax.random.key(seed), 16)
    moe_input = noise(seeds[0], (TOKENS, D), 1.0, 6.0, ((0, 8),))
    out_cotangent = gaussian_with(seeds[1], (TOKENS, D), 1.0, 6.0, ((0, 8),), (0, 1, 8, 2.0))
    routes_keys = jax.random.split(jax.random.fold_in(seeds[2], 1), TOKENS // TOK_DEV)
    routes_turns = jax.random.permutation(jax.random.fold_in(seeds[2], 3), TOKENS // TOK_DEV)
    routes = jax.vmap(lambda own, number: deal_out(jax.random.fold_in(seeds[2], 2), own, number, TOK_DEV, EXPERTS, 2, CAP, 2))(routes_keys, routes_turns).reshape((TOKENS, 2))
    group_weight = jnp.clip(0.5 + 0.5 * jax.random.uniform(seeds[3], (TOKENS,), jnp.float32) ** steps_of(seeds[3], (TOKENS,), ((0, 8),), -0.2, 0.2), 0.5, 1.0)
    inner_weight = jnp.clip(0.3 + 0.7 * jax.random.uniform(seeds[4], (TOKENS, 2), jnp.float32) ** steps_of(seeds[4], (TOKENS, 2), ((0, 8),), -0.2, 0.2), 0.3, 1.0)
    gate_weight = noise(seeds[5], (EXPERTS, D, FF), D ** -0.5, 0.125, ((0, 8), (2, 4)))
    up_weight = noise(seeds[6], (EXPERTS, D, FF), D ** -0.5, 0.125, ((0, 8), (2, 4)))
    down_weight = noise(seeds[7], (EXPERTS, FF, D), FF ** -0.5, 0.1875, ((0, 8), (1, 4)))
    value_in = noise(seeds[8], (TOKENS, CONV), 1.0, 6.0, ((0, 8), (1, 4)))
    gate_in = noise(seeds[9], (TOKENS, CONV), 1.0, 6.0, ((0, 8), (1, 4)))
    conv_taps = noise(seeds[10], (KERNEL, CONV), KERNEL ** -0.5, 1.0, ((1, 4),))
    norm_hat = noise(seeds[11], (TOKENS, CONV), 1.0, 6.0, ((0, 8), (1, 4)))
    norm_rstd = jnp.clip(jnp.exp(math.log(3.0) - 2.3025851 * jax.random.uniform(seeds[12], (TOKENS,), jnp.float32) ** steps_of(seeds[12], (TOKENS,), ((0, 8),), -0.2, 0.2)), 0.3, 3.0)
    norm_gain = jnp.clip(1.0 + 0.18 * jax.random.normal(seeds[13], (CONV,), jnp.float32), 0.1, 1.9)
    out_proj = noise(seeds[14], (D, CONV), CONV ** -0.5, 0.1875, ((1, 4),))
    return dict(moe_input=moe_input, out_cotangent=out_cotangent, routes=routes, group_weight=group_weight, inner_weight=inner_weight, gate_weight=gate_weight, up_weight=up_weight, down_weight=down_weight, value_in=value_in, gate_in=gate_in, conv_taps=conv_taps, norm_hat=norm_hat, norm_rstd=norm_rstd, norm_gain=norm_gain, out_proj=out_proj)


def round_half(values):
    return lax.optimization_barrier(values.astype(jnp.bfloat16)).astype(jnp.float32)


def silu_slope(logits, squashed):
    return squashed * (1.0 + logits * (1.0 - squashed))


def reference(moe_input, out_cotangent, routes, group_weight, inner_weight, gate_weight, up_weight, down_weight, value_in, gate_in, conv_taps, norm_hat, norm_rstd, norm_gain, out_proj):
    tok_total, model_width = moe_input.shape
    all_experts = gate_weight.shape[0]
    hidden_units = gate_weight.shape[2]
    block_count = tok_total // TOK_DEV
    block_routes = 2 * TOK_DEV
    total_routes = 2 * tok_total
    routes_flat = routes.reshape(block_count, block_routes).astype(jnp.int32)
    one_hot = (routes_flat[:, :, None] == jnp.arange(all_experts, dtype=jnp.int32)[None, None, :]).astype(jnp.int32)
    slot_rank = jnp.sum(one_hot * (jnp.cumsum(one_hot, axis=1) - one_hot), axis=2)
    expert_rows = block_count * CAP
    slot_index = routes_flat * expert_rows + jnp.arange(block_count, dtype=jnp.int32)[:, None] * CAP + slot_rank
    slot_index = slot_index.reshape(total_routes).astype(jnp.int32)
    slot_owner = jnp.full((all_experts * expert_rows,), total_routes, jnp.int32).at[slot_index].set(jnp.arange(total_routes, dtype=jnp.int32))
    route_weight = group_weight[:, None] * inner_weight
    scaled = (route_weight[:, :, None] * out_cotangent.astype(jnp.float32)[:, None, :]).astype(jnp.bfloat16)
    scaled = jnp.concatenate([scaled.reshape(total_routes, model_width), jnp.zeros((1, model_width), jnp.bfloat16)])
    inputs = jnp.concatenate([moe_input, jnp.zeros((1, model_width), jnp.bfloat16)])
    owners = slot_owner.reshape(all_experts, expert_rows)
    quarter = hidden_units // N_TP

    def one_expert(packed):
        w_gate, w_up, w_down, members = packed
        slot_grad = scaled[members]
        slot_input = inputs[members // 2]
        gate_pre = jnp.dot(slot_input, w_gate, preferred_element_type=jnp.float32)
        up_pre = jnp.dot(slot_input, w_up, preferred_element_type=jnp.float32)
        gate_sigma = jax.nn.sigmoid(gate_pre)
        hidden_act = (gate_pre * gate_sigma * up_pre).astype(jnp.bfloat16)
        act_grad = jnp.dot(slot_grad, w_down.T, preferred_element_type=jnp.float32)
        gate_delta = (act_grad * up_pre * silu_slope(gate_pre, gate_sigma)).astype(jnp.bfloat16)
        up_delta = (act_grad * gate_pre * gate_sigma).astype(jnp.bfloat16)
        down_part = jnp.dot(hidden_act.T, slot_grad, preferred_element_type=jnp.float32).astype(jnp.bfloat16)
        gate_part = jnp.dot(slot_input.T, gate_delta, preferred_element_type=jnp.float32).astype(jnp.bfloat16)
        up_part = jnp.dot(slot_input.T, up_delta, preferred_element_type=jnp.float32).astype(jnp.bfloat16)
        summed = jnp.zeros((members.shape[0], model_width), jnp.float32)
        for block in range(N_TP):
            lower = block * quarter
            upper = lower + quarter
            partial_value = jnp.dot(gate_delta[:, lower:upper], w_gate[:, lower:upper].T, preferred_element_type=jnp.float32)
            partial_value = partial_value + jnp.dot(up_delta[:, lower:upper], w_up[:, lower:upper].T, preferred_element_type=jnp.float32)
            summed = summed + round_half(partial_value)
        return gate_part, up_part, down_part, summed.astype(jnp.bfloat16)

    gate_grad, up_grad, down_grad, slot_back = lax.map(one_expert, (gate_weight, up_weight, down_weight, owners))
    route_back = slot_back.reshape(all_experts * expert_rows, model_width)[slot_index]
    returned = jnp.sum(route_back.reshape(tok_total, 2, model_width).astype(jnp.float32), axis=1)
    mixer_grad = (out_cotangent.astype(jnp.float32) + returned).astype(jnp.bfloat16)
    normed = norm_hat.astype(jnp.float32) * norm_gain[None, :]
    norm_sigma = jax.nn.sigmoid(normed)
    mixer_act = (normed * norm_sigma).astype(jnp.bfloat16)
    proj_grad = jnp.dot(mixer_grad.T, mixer_act, preferred_element_type=jnp.float32)
    silu_grad = jnp.dot(mixer_grad, out_proj, preferred_element_type=jnp.float32)
    hat_grad = silu_grad * silu_slope(normed, norm_sigma) * norm_gain[None, :]
    norm_values = norm_hat.astype(jnp.float32)
    grad_mean = jnp.mean(hat_grad, axis=1, keepdims=True)
    grad_dot = jnp.mean(hat_grad * norm_values, axis=1, keepdims=True)
    conv_grad = norm_rstd[:, None] * (hat_grad - grad_mean - norm_values * grad_dot)
    tap_count = conv_taps.shape[0]
    extended = jnp.pad(conv_grad, ((0, tap_count - 1), (0, 0)))
    tap_values = conv_taps.astype(jnp.float32)
    glu_grad = jnp.zeros_like(conv_grad)
    for offset in range(tap_count):
        lower = tap_count - 1 - offset
        glu_grad = glu_grad + tap_values[offset][None, :] * extended[lower:lower + tok_total]
    gate_sigma = jax.nn.sigmoid(gate_in.astype(jnp.float32))
    value_grad = (glu_grad * gate_sigma).astype(jnp.bfloat16)
    gate_in_grad = (glu_grad * value_in.astype(jnp.float32) * gate_sigma * (1.0 - gate_sigma)).astype(jnp.bfloat16)
    return gate_grad, up_grad, down_grad, proj_grad, value_grad, gate_in_grad
```

```python
import functools

import jax
import jax.numpy as jnp
from jax import lax
from jax.experimental import pallas as pl
from jax.experimental.pallas import tpu as pltpu
from jax.sharding import PartitionSpec as P


F32 = jnp.float32
BF16 = jnp.bfloat16
VMEM = pl.BlockSpec(memory_space=pltpu.VMEM)
SMEM = pl.BlockSpec(memory_space=pltpu.SMEM)


def swapped(block, axis, mask):
    count = lax.axis_size(axis)
    return lax.ppermute(block, axis, [(i, i ^ mask) for i in range(count)])


def shifted(block, axis, distance):
    devices = range(lax.axis_size(axis))
    route = [(i - distance, i) for i in devices if i - distance in devices]
    return lax.ppermute(block, axis, route)


def groups_of(count):
    if count == 8:
        return [[0, 1, 2], [3, 4], [5, 6], [7]]
    return None


def silu_slope(logits, squashed):
    return squashed * (1.0 + logits * (1.0 - squashed))


def dot(a, b, contract):
    return lax.dot_general(a, b, ((contract[:1], contract[1:]), ((), ())), preferred_element_type=F32)


def params(mib):
    return pltpu.CompilerParams(vmem_limit_bytes=mib * 1024 * 1024)


def dispatch_kernel(
    experts, capacity, flip, pos, routes, group, inner, x_ref, g_ref, select_ref, *slot_refs
):
    tokens = routes.shape[1]
    slots = experts * capacity
    expert = lax.broadcasted_iota(jnp.int32, (experts, tokens), 0)
    earlier = lax.broadcasted_iota(jnp.int32, (tokens, tokens), 0)
    later = lax.broadcasted_iota(jnp.int32, (tokens, tokens), 1)
    before = (earlier < later).astype(F32).astype(BF16)
    slot_number = lax.broadcasted_iota(jnp.int32, (slots, tokens), 0)
    base = jnp.zeros((experts, 1), F32)
    select = jnp.zeros((slots, tokens), F32)
    weight = jnp.zeros((slots, tokens), F32)
    for k in range(2):
        route = routes[k : k + 1, :]
        hot = (expert == route).astype(F32)
        counts = dot(hot.astype(BF16), before, (1, 0)) + base
        base = base + jnp.sum(hot, axis=1, keepdims=True)
        rank = jnp.sum(hot * counts, axis=0, keepdims=True).astype(jnp.int32)
        owner = jnp.bitwise_xor(route, pos[1]) if flip else route
        hit = slot_number == owner * capacity + rank
        select = jnp.where(hit, 1.0, select)
        weight = jnp.where(hit, group[...] * inner[k : k + 1, :], weight)
    select = select.astype(BF16)
    select_ref[...] = select
    weight = jnp.sum(weight, axis=1, keepdims=True)
    width = x_ref.shape[1]
    rows = slots // len(slot_refs)
    picked_x = dot(select, x_ref[...], (1, 0)).astype(BF16)
    picked_g = (weight * dot(select, g_ref[...], (1, 0))).astype(BF16)
    for i, out in enumerate(slot_refs):
        out[:, :width] = picked_x[i * rows : (i + 1) * rows]
        out[:, width:] = picked_g[i * rows : (i + 1) * rows]


def dispatch(pos, routes, group_weight, inner_weight, x, g, experts, capacity, parts):
    tokens, model = x.shape
    width = model // lax.axis_size("tp")
    slots = experts * capacity
    rows = slots // parts
    whole = lambda *shape: pl.BlockSpec(shape, lambda i, pos: (0,) * len(shape))
    columns = pl.BlockSpec((tokens, width), lambda i, pos: (0, pos[0]))
    return pl.pallas_call(
        functools.partial(dispatch_kernel, experts, capacity, parts > 1),
        grid_spec=pltpu.PrefetchScalarGridSpec(
            num_scalar_prefetch=1,
            grid=(1,),
            in_specs=[whole(2, tokens), whole(1, tokens), whole(2, tokens), columns, columns],
            out_specs=[whole(slots, tokens)] + [whole(rows, 2 * width)] * parts,
        ),
        out_shape=[jax.ShapeDtypeStruct((slots, tokens), BF16)]
        + [jax.ShapeDtypeStruct((rows, 2 * width), BF16)] * parts,
        compiler_params=params(24),
        name="dispatch",
    )(pos, routes.T, group_weight[None, :], inner_weight.T, x, g)


def quarters(pos):
    p = pos[0]
    return [p, jnp.bitwise_xor(p, 2), jnp.bitwise_xor(p, 1), jnp.bitwise_xor(p, 3)]


def expert_kernel(pos, own, far, mate, mate_far, wg, wu, wd, send, keep, keep_far, gd, ud, ha):
    rows, double = own.shape
    width = double // 2
    order = [pl.multiple_of(q * width, width) for q in quarters(pos)]
    hidden = wg.shape[1]
    gate = jnp.zeros((rows, hidden), F32)
    up = jnp.zeros((rows, hidden), F32)
    act = jnp.zeros((rows, hidden), F32)
    for buf, at in zip((own, far, mate, mate_far), order):
        part = buf[:, :width]
        gate = gate + dot(part, wg[pl.ds(at, width), :], (1, 0))
        up = up + dot(part, wu[pl.ds(at, width), :], (1, 0))
        act = act + dot(buf[:, width:], wd[:, pl.ds(at, width)], (1, 1))
    sigma = jax.nn.sigmoid(gate)
    ha[...] = (gate * sigma * up).astype(BF16)
    gate_delta = (act * up * silu_slope(gate, sigma)).astype(BF16)
    up_delta = (act * gate * sigma).astype(BF16)
    gd[...] = gate_delta
    ud[...] = up_delta

    def partial_of(at):
        value = dot(gate_delta, wg[pl.ds(at, width), :], (1, 1))
        value = value + dot(up_delta, wu[pl.ds(at, width), :], (1, 1))
        return value.astype(BF16)

    send[:, :width] = partial_of(order[2])
    send[:, width:] = partial_of(order[3])
    keep[...] = partial_of(order[0])
    keep_far[...] = partial_of(order[1])


def expert_math(pos, bufs, wg, wu, wd):
    rows, double = bufs[0].shape
    width = double // 2
    hidden = wg.shape[1]
    shape = lambda w: jax.ShapeDtypeStruct((rows, w), BF16)
    return pl.pallas_call(
        expert_kernel,
        in_specs=[SMEM] + [VMEM] * 7,
        out_specs=[VMEM] * 6,
        out_shape=[shape(double), shape(width), shape(width)] + [shape(hidden)] * 3,
        compiler_params=params(24),
        name="expert",
    )(pos, *bufs, wg, wu, wd)


def weight_kernel(groups, pos, *refs):
    ins, (gate_grad, up_grad, down_grad) = refs[: 7 * groups], refs[7 * groups :]
    width = ins[0].shape[1] // 2
    hidden = gate_grad.shape[1]
    order = [pl.multiple_of(q * width, width) for q in quarters(pos)]
    for which in range(4):
        at = order[which]
        gate = jnp.zeros((width, hidden), F32)
        up = jnp.zeros((width, hidden), F32)
        down = jnp.zeros((hidden, width), F32)
        for i in range(groups):
            buf = ins[7 * i + which]
            gd, ud, ha = ins[7 * i + 4 : 7 * i + 7]
            part = buf[:, :width]
            gate = gate + dot(part, gd[...], (0, 0))
            up = up + dot(part, ud[...], (0, 0))
            down = down + dot(ha[...], buf[:, width:], (0, 0))
        gate_grad[pl.ds(at, width), :] = gate.astype(BF16)
        up_grad[pl.ds(at, width), :] = up.astype(BF16)
        down_grad[:, pl.ds(at, width)] = down.astype(BF16)


def weight_math(pos, flat, model, hidden):
    groups = len(flat) // 7
    return pl.pallas_call(
        functools.partial(weight_kernel, groups),
        in_specs=[SMEM] + [VMEM] * len(flat),
        out_specs=[VMEM] * 3,
        out_shape=[
            jax.ShapeDtypeStruct((model, hidden), BF16),
            jax.ShapeDtypeStruct((model, hidden), BF16),
            jax.ShapeDtypeStruct((hidden, model), BF16),
        ],
        compiler_params=params(32),
        name="weights",
    )(pos, *flat)


def combine_kernel(pos, select, g_ref, *refs):
    blocks, (out, rows) = refs[:-2], refs[-2:]
    at = 0
    for block in blocks:
        rows[at : at + block.shape[0], :] = block[...]
        at += block.shape[0]
    out[...] = (g_ref[...].astype(F32) + dot(select[...], rows[...], (0, 0))).astype(BF16)


def combine(pos, select, g, blocks):
    slots, tokens = select.shape
    width = blocks[0].shape[1]
    whole = lambda a: pl.BlockSpec(a.shape, lambda i, pos: (0,) * a.ndim)
    return pl.pallas_call(
        combine_kernel,
        grid_spec=pltpu.PrefetchScalarGridSpec(
            num_scalar_prefetch=1,
            grid=(1,),
            in_specs=[whole(select), pl.BlockSpec((tokens, width), lambda i, pos: (0, pos[0]))]
            + [whole(b) for b in blocks],
            out_specs=pl.BlockSpec((tokens, width), lambda i, pos: (0, 0)),
            scratch_shapes=[pltpu.VMEM((slots, width), BF16)],
        ),
        out_shape=jax.ShapeDtypeStruct((tokens, width), BF16),
        compiler_params=params(16),
        name="combine",
    )(pos, select, g, *blocks)


def project_kernel(pos, own, far, mate, mate_far, hat, gain, mixer, *refs):
    outs, total = refs[:-1], refs[-1]
    width = own.shape[1]
    order = [pl.multiple_of(q * width, width) for q in quarters(pos)]
    normed = hat[...].astype(F32) * gain[...]
    act = (normed * jax.nn.sigmoid(normed)).astype(BF16)
    for buf, at in zip((own, far, mate, mate_far), order):
        part = buf[...]
        mixer[:, pl.ds(at, width)] = part
        total[pl.ds(at, width), :] = dot(part, act, (0, 0))
    if len(outs) == 1:
        outs[0][...] = total[...].astype(BF16)
        return
    for i, out in enumerate(outs):
        rows = out.shape[0]
        block = jnp.bitwise_xor(pos[1], i) * rows
        out[...] = total[pl.ds(pl.multiple_of(block, rows), rows), :].astype(out.dtype)


def project(pos, bufs, norm_hat, norm_gain, parts):
    tokens, width = bufs[0].shape
    model = width * lax.axis_size("tp")
    channels = norm_hat.shape[1]
    rows = model // parts
    kinds = [BF16] if parts == 1 else [F32] + [BF16] * (parts - 1)
    return pl.pallas_call(
        project_kernel,
        in_specs=[SMEM] + [VMEM] * 6,
        out_specs=[VMEM] * (1 + parts),
        out_shape=[jax.ShapeDtypeStruct((tokens, model), BF16)]
        + [jax.ShapeDtypeStruct((rows, channels), kind) for kind in kinds],
        scratch_shapes=[pltpu.VMEM((model, channels), F32)],
        compiler_params=params(16),
        name="project",
    )(pos, *bufs, norm_hat, norm_gain[None, :])


def gathered(own):
    far = swapped(own, "tp", 2)
    return own, far, swapped(own, "tp", 1), swapped(far, "tp", 1)


def added(a, b):
    return a.astype(F32) + b.astype(F32)


def on_device(
    moe_input,
    out_cotangent,
    routes,
    group_weight,
    inner_weight,
    gate_weight,
    up_weight,
    down_weight,
    value_in,
    gate_in,
    conv_taps,
    norm_hat,
    norm_rstd,
    norm_gain,
    out_proj,
):
    tok_rows, model_width = moe_input.shape
    local_experts = gate_weight.shape[0]
    sp_count = lax.axis_size("sp")
    tp_count = lax.axis_size("tp")
    if local_experts != 1 or tp_count != 4:
        raise ValueError("unsupported mesh")
    capacity = 3 * tok_rows // sp_count
    col_width = model_width // tp_count
    wg, wu, wd = gate_weight[0], up_weight[0], down_weight[0]
    hidden = wg.shape[1]
    pos = jnp.stack([lax.axis_index("tp"), lax.axis_index("sp")]).astype(jnp.int32)
    groups = groups_of(sp_count)
    parts = sp_count if groups else 1
    select, *slots = dispatch(
        pos,
        routes,
        group_weight,
        inner_weight,
        moe_input,
        out_cotangent,
        sp_count,
        capacity,
        parts,
    )
    if groups:
        arrived = [slots[0]] + [swapped(slots[d], "sp", d) for d in range(1, parts)]
        grouped = [jnp.concatenate([arrived[d] for d in group]) for group in groups]
    else:
        block = slots[0].reshape(sp_count, capacity, 2 * col_width)
        block = lax.all_to_all(block, "sp", split_axis=0, concat_axis=0, tiled=True)
        grouped = [block.reshape(sp_count * capacity, 2 * col_width)]
    returned = [None] * sp_count
    flat = []
    for i, own in enumerate(grouped):
        bufs = gathered(own)
        send, keep, keep_far, gd, ud, ha = expert_math(pos, bufs, wg, wu, wd)
        flat.extend(bufs + (gd, ud, ha))
        mate = swapped(send, "tp", 1)
        to_far = added(keep_far, mate[:, col_width:]).astype(BF16)
        half = added(keep, mate[:, :col_width])
        total = added(half, swapped(to_far, "tp", 2)).astype(BF16)
        if groups:
            for j, d in enumerate(groups[i]):
                block = total[j * capacity : (j + 1) * capacity]
                returned[d] = swapped(block, "sp", d) if d else block
        else:
            block = total.reshape(sp_count, capacity, col_width)
            block = lax.all_to_all(block, "sp", split_axis=0, concat_axis=0, tiled=True)
            returned = [block.reshape(sp_count * capacity, col_width)]
    gate_grad, up_grad, down_grad = weight_math(pos, flat, model_width, hidden)
    mixer_part = combine(pos, select, out_cotangent, returned)
    mixer_grad, *blocks = project(pos, gathered(mixer_part), norm_hat, norm_gain, parts)
    if groups:
        proj_grad = blocks[0]
        for d in range(1, parts):
            proj_grad = proj_grad + swapped(blocks[d], "sp", d).astype(F32)
    else:
        block = blocks[0].reshape(sp_count, model_width // sp_count, -1)
        block = lax.all_to_all(block, "sp", split_axis=0, concat_axis=0, tiled=True)
        proj_grad = jnp.sum(block.astype(F32), axis=0)
    normed = norm_hat.astype(F32) * norm_gain[None, :]
    norm_sigma = jax.nn.sigmoid(normed)
    silu_grad = jnp.dot(mixer_grad, out_proj, preferred_element_type=F32)
    hat_grad = silu_grad * silu_slope(normed, norm_sigma) * norm_gain[None, :]
    norm_values = norm_hat.astype(F32)
    grad_sum, grad_dot = lax.psum(
        (jnp.sum(hat_grad, axis=1), jnp.sum(hat_grad * norm_values, axis=1)), "tp"
    )
    channels = norm_values.shape[1] * tp_count
    conv_grad = norm_rstd[:, None] * (
        hat_grad - grad_sum[:, None] / channels - norm_values * (grad_dot[:, None] / channels)
    )
    tap_count = conv_taps.shape[0]
    incoming = shifted(conv_grad[: tap_count - 1], "sp", -1)
    extended = jnp.concatenate([conv_grad, incoming], axis=0)
    tap_values = conv_taps.astype(F32)
    glu_grad = jnp.zeros_like(conv_grad)
    for offset in range(tap_count):
        lower = tap_count - 1 - offset
        glu_grad = glu_grad + tap_values[offset][None, :] * extended[lower : lower + tok_rows]
    input_sigma = jax.nn.sigmoid(gate_in.astype(F32))
    value_grad = (glu_grad * input_sigma).astype(BF16)
    gate_in_grad = (
        glu_grad * value_in.astype(F32) * input_sigma * (1.0 - input_sigma)
    ).astype(BF16)
    return (gate_grad[None], up_grad[None], down_grad[None], proj_grad, value_grad, gate_in_grad)


def solution(mesh):
    return jax.shard_map(
        on_device,
        mesh=mesh,
        in_specs=(
            P("sp", None),
            P("sp", None),
            P("sp", None),
            P("sp"),
            P("sp", None),
            P("sp", None, "tp"),
            P("sp", None, "tp"),
            P("sp", "tp", None),
            P("sp", "tp"),
            P("sp", "tp"),
            P(None, "tp"),
            P("sp", "tp"),
            P("sp"),
            P("tp"),
            P(None, "tp"),
        ),
        out_specs=(
            P("sp", None, "tp"),
            P("sp", None, "tp"),
            P("sp", "tp", None),
            P("sp", "tp"),
            P("sp", "tp"),
            P("sp", "tp"),
        ),
        check_vma=False,
    )
```

```python
import functools

import jax
import jax.numpy as jnp
from jax import lax
from jax.experimental import pallas as pl
from jax.experimental.pallas import tpu as pltpu
from jax.sharding import PartitionSpec as P


F32 = jnp.float32
BF16 = jnp.bfloat16
VMEM = pl.BlockSpec(memory_space=pltpu.VMEM)
SMEM = pl.BlockSpec(memory_space=pltpu.SMEM)
HBM = pl.BlockSpec(memory_space=pltpu.HBM)


WIDE = 3
GROUPS = {"a": ((0, 1, 2), ()), "b": ((4,), (3, 5)), "c": ((), (6, 7))}
PLACES = sum((g[0] for g in GROUPS.values()), ()) + sum((g[1] for g in GROUPS.values()), ())
SENT = ((5, 7), (1, 3), (4, 6), (0, 2))


def swapped(block, axis, mask):
    count = lax.axis_size(axis)
    return lax.ppermute(block, axis, [(i, i ^ mask) for i in range(count)])


def shifted(block, axis, distance):
    devices = range(lax.axis_size(axis))
    route = [(i - distance, i) for i in devices if i - distance in devices]
    return lax.ppermute(block, axis, route)


def silu_slope(logits, squashed):
    return squashed * (1.0 + logits * (1.0 - squashed))


def dot(a, b, contract):
    return lax.dot_general(a, b, ((contract[:1], contract[1:]), ((), ())), preferred_element_type=F32)


def params(mib):
    return pltpu.CompilerParams(vmem_limit_bytes=mib * 1024 * 1024)


def array(*shape, kind=BF16):
    return jax.ShapeDtypeStruct(shape, kind)


def in_hbm(*arrays):
    return [pltpu.with_memory_space_constraint(a, pltpu.HBM) for a in arrays]


def dispatch_kernel(
    experts, capacity, wide, flip, pos, routes_in, group_in, inner_in, x_all, g_all, select_ref, g_own, *refs
):
    slot_refs, (x_own, x_far, g_far, routes, group, inner, sems) = refs[:-7], refs[-7:]
    tables = [
        pltpu.make_async_copy(source, target, sems.at[4 + i])
        for i, (source, target) in enumerate(
            ((routes_in, routes), (group_in, group), (inner_in, inner))
        )
    ]
    for copy in tables:
        copy.start()
    width = x_own.shape[1]

    def fetch(source, target, quarter, i):
        at = pl.ds(pl.multiple_of(quarter * width, width), width)
        return pltpu.make_async_copy(source.at[:, at], target, sems.at[i])

    far = jnp.bitwise_xor(pos[0], 2)
    copies = [fetch(x_all, x_own, pos[0], 0), fetch(g_all, g_own, pos[0], 1)]
    if wide:
        copies += [fetch(x_all, x_far, far, 2), fetch(g_all, g_far, far, 3)]
    for copy in copies:
        copy.start()
    for copy in tables:
        copy.wait()
    tokens = routes.shape[1]
    slots = experts * capacity
    expert = lax.broadcasted_iota(jnp.int32, (experts, tokens), 0)
    earlier = lax.broadcasted_iota(jnp.int32, (tokens, tokens), 0)
    later = lax.broadcasted_iota(jnp.int32, (tokens, tokens), 1)
    before = (earlier < later).astype(F32).astype(BF16)
    slot_number = lax.broadcasted_iota(jnp.int32, (slots, tokens), 0)
    base = jnp.zeros((experts, 1), F32)
    select = jnp.zeros((slots, tokens), F32)
    weight = jnp.zeros((slots, tokens), F32)
    for k in range(2):
        route = routes[k : k + 1, :]
        hot = (expert == route).astype(F32)
        counts = dot(hot.astype(BF16), before, (1, 0)) + base
        base = base + jnp.sum(hot, axis=1, keepdims=True)
        rank = jnp.sum(hot * counts, axis=0, keepdims=True).astype(jnp.int32)
        owner = route
        if flip:
            mask = jnp.bitwise_xor(route, pos[1])
            owner = mask
            for place, own in enumerate(PLACES):
                if place != own:
                    owner = jnp.where(mask == own, place, owner)
        hit = slot_number == owner * capacity + rank
        select = jnp.where(hit, 1.0, select)
        weight = jnp.where(hit, group[...] * inner[k : k + 1, :], weight)
    select = select.astype(BF16)
    select_ref[...] = select
    weight = jnp.sum(weight, axis=1, keepdims=True)
    rows = slots // len(slot_refs)
    for copy in copies:
        copy.wait()
    picked_x = dot(select, x_own[...], (1, 0)).astype(BF16)
    picked_g = (weight * dot(select, g_own[...], (1, 0))).astype(BF16)
    for i, out in enumerate(slot_refs):
        out[:, :width] = picked_x[i * rows : (i + 1) * rows]
        out[:, width : 2 * width] = picked_g[i * rows : (i + 1) * rows]
    if wide:
        select, weight = select[: wide * rows], weight[: wide * rows]
        picked_x = dot(select, x_far[...], (1, 0)).astype(BF16)
        picked_g = (weight * dot(select, g_far[...], (1, 0))).astype(BF16)
        for i, out in enumerate(slot_refs[:wide]):
            out[:, 2 * width : 3 * width] = picked_x[i * rows : (i + 1) * rows]
            out[:, 3 * width :] = picked_g[i * rows : (i + 1) * rows]


def dispatch(pos, routes, group_weight, inner_weight, x, g, experts, capacity, parts, wide):
    tokens, model = x.shape
    width = model // lax.axis_size("tp")
    slots = experts * capacity
    rows = slots // parts
    return pl.pallas_call(
        functools.partial(dispatch_kernel, experts, capacity, wide, parts > 1),
        in_specs=[SMEM] + [HBM] * 5,
        out_specs=[VMEM] * (2 + parts),
        out_shape=[array(slots, tokens), array(tokens, width)]
        + [array(rows, (4 if i < wide else 2) * width) for i in range(parts)],
        scratch_shapes=[pltpu.VMEM((tokens, width), BF16)] * 3
        + [
            pltpu.VMEM((2, tokens), jnp.int32),
            pltpu.VMEM((1, tokens), F32),
            pltpu.VMEM((2, tokens), F32),
            pltpu.SemaphoreType.DMA((7,)),
        ],
        compiler_params=params(20),
        name="dispatch",
    )(pos, *in_hbm(routes.T, group_weight[None, :], inner_weight.T, x, g))


def quarters(pos, width):
    p = pos[0]
    order = [p, jnp.bitwise_xor(p, 2), jnp.bitwise_xor(p, 1), jnp.bitwise_xor(p, 3)]
    return [pl.multiple_of(q * width, width) for q in order]


def expert_kernel(layout, fetch, pos, *refs):
    if fetch:
        refs, (fetched, sem) = refs[:-2], refs[-2:]
    ins, (wg, wu, wd, both, send, keep, gd, ud, ha) = refs[:-9], refs[-9:]
    if fetch:
        copy = pltpu.make_async_copy(wd, fetched, sem)
        copy.start()
    width = keep.shape[1] // 2
    model = both.shape[1] // 2
    order = quarters(pos, width)
    for ref, (row, which) in zip(ins, layout):
        rows = slice(row, row + ref.shape[0])
        for i in range(ref.shape[1] // (2 * width)):
            at = order[which + i]
            lower = 2 * i * width
            both[rows, pl.ds(at, width)] = ref[:, lower : lower + width]
            at = pl.multiple_of(model + at, width)
            both[rows, pl.ds(at, width)] = ref[:, lower + width : lower + 2 * width]
    gate = dot(both[:, :model], wg[...], (1, 0))
    up = dot(both[:, :model], wu[...], (1, 0))
    if fetch:
        copy.wait()
        wd = fetched
    act = dot(both[:, model:], wd[...], (1, 1))
    sigma = jax.nn.sigmoid(gate)
    ha[...] = (gate * sigma * up).astype(BF16)
    gate_delta = (act * up * silu_slope(gate, sigma)).astype(BF16)
    up_delta = (act * gate * sigma).astype(BF16)
    gd[...] = gate_delta
    ud[...] = up_delta

    def partial_of(at):
        value = dot(gate_delta, wg[pl.ds(at, width), :], (1, 1))
        value = value + dot(up_delta, wu[pl.ds(at, width), :], (1, 1))
        return value.astype(BF16)

    send[:, :width] = partial_of(order[2])
    send[:, width:] = partial_of(order[3])
    keep[:, :width] = partial_of(order[0])
    keep[:, width:] = partial_of(order[1])


def expert_math(pos, blocks, layout, rows, wg, wu, wd, fetch):
    model, hidden = wg.shape
    width = model // lax.axis_size("tp")
    return pl.pallas_call(
        functools.partial(expert_kernel, layout, fetch),
        in_specs=[SMEM] + [VMEM] * (len(blocks) + 2) + [HBM if fetch else VMEM],
        out_specs=[VMEM] * 6,
        out_shape=[array(rows, 2 * model)]
        + [array(rows, 2 * width)] * 2
        + [array(rows, hidden)] * 3,
        scratch_shapes=[pltpu.VMEM(wd.shape, BF16), pltpu.SemaphoreType.DMA] if fetch else [],
        compiler_params=params(20),
        name="expert",
    )(pos, *blocks, wg, wu, *(in_hbm(wd) if fetch else [wd]))


def weight_kernel(groups, *refs):
    ins, (gate_grad, up_grad, down_grad) = refs[: 4 * groups], refs[4 * groups :]
    model = gate_grad.shape[0]
    hidden = gate_grad.shape[1]
    width = model // 4
    for at in range(0, model, width):
        gate = jnp.zeros((width, hidden), F32)
        up = jnp.zeros((width, hidden), F32)
        down = jnp.zeros((hidden, width), F32)
        for i in range(groups):
            both, gd, ud, ha = ins[4 * i : 4 * i + 4]
            part = both[:, at : at + width]
            gate = gate + dot(part, gd[...], (0, 0))
            up = up + dot(part, ud[...], (0, 0))
            down = down + dot(ha[...], both[:, model + at : model + at + width], (0, 0))
        gate_grad[at : at + width, :] = gate.astype(BF16)
        up_grad[at : at + width, :] = up.astype(BF16)
        down_grad[:, at : at + width] = down.astype(BF16)


def weight_math(flat, model, hidden):
    return pl.pallas_call(
        functools.partial(weight_kernel, len(flat) // 4),
        in_specs=[VMEM] * len(flat),
        out_specs=[VMEM] * 3,
        out_shape=[array(model, hidden), array(model, hidden), array(hidden, model)],
        compiler_params=params(20),
        name="weights",
    )(*flat)


def join_kernel(keep, mate, *outs):
    row = 0
    for out in outs:
        rows = slice(row, row + out.shape[0])
        out[...] = (keep[rows, :].astype(F32) + mate[rows, :].astype(F32)).astype(BF16)
        row += out.shape[0]


def join(keep, mate, rows, parts):
    return pl.pallas_call(
        join_kernel,
        in_specs=[VMEM] * 2,
        out_specs=[VMEM] * parts,
        out_shape=[array(rows, keep.shape[1])] * parts,
        compiler_params=params(12),
        name="join",
    )(keep, mate)


def fold_kernel(start, keep, mate, half, far):
    width = half.shape[1]
    half[...] = keep[start:, :width].astype(F32) + mate[start:, :width].astype(F32)
    far[...] = (keep[start:, width:].astype(F32) + mate[start:, width:].astype(F32)).astype(BF16)


def fold(keep, mate, start):
    rows, double = keep.shape
    shape = (rows - start, double // 2)
    return pl.pallas_call(
        functools.partial(fold_kernel, start),
        in_specs=[VMEM] * 2,
        out_specs=[VMEM] * 2,
        out_shape=[array(*shape, kind=F32), array(*shape)],
        compiler_params=params(12),
        name="fold",
    )(keep, mate)


def stacked(blocks, rows):
    at = 0
    for block in blocks:
        rows[at : at + block.shape[0], :] = block[...]
        at += block.shape[0]


def early_kernel(select, *refs):
    blocks, (keep, far, rows) = refs[:-3], refs[-3:]
    stacked(blocks, rows)
    width = keep.shape[1]
    total = dot(select[: rows.shape[0], :], rows[...], (0, 0))
    keep[...] = total[:, :width]
    far[...] = total[:, width:].astype(BF16)


def early(select, blocks):
    tokens = select.shape[1]
    rows = sum(b.shape[0] for b in blocks)
    width = blocks[0].shape[1] // 2
    return pl.pallas_call(
        early_kernel,
        in_specs=[VMEM] * (1 + len(blocks)),
        out_specs=[VMEM] * 2,
        out_shape=[array(tokens, width, kind=F32), array(tokens, width)],
        scratch_shapes=[pltpu.VMEM((rows, 2 * width), BF16)],
        compiler_params=params(12),
        name="early",
    )(select, *blocks)


def combine_kernel(count, select, g_own, *refs):
    blocks, others, (out, rows) = refs[:count], refs[count:-2], refs[-2:]
    stacked(blocks, rows)
    total = dot(select[select.shape[0] - rows.shape[0] :, :], rows[...], (0, 0))
    for other in others:
        total = total + other[...].astype(F32)
    out[...] = (g_own[...].astype(F32) + total).astype(BF16)


def combine(select, g, blocks, others):
    tokens = select.shape[1]
    width = blocks[0].shape[1]
    rows = sum(b.shape[0] for b in blocks)
    return pl.pallas_call(
        functools.partial(combine_kernel, len(blocks)),
        in_specs=[VMEM] * (2 + len(blocks) + len(others)),
        out_specs=VMEM,
        out_shape=array(tokens, width),
        scratch_shapes=[pltpu.VMEM((rows, width), BF16)],
        compiler_params=params(12),
        name="combine",
    )(select, g, *blocks, *others)


def project_kernel(pos, own, far, mate, mate_far, hat, gain, mixer, *refs):
    outs, total = refs[:-1], refs[-1]
    width = own.shape[1]
    normed = hat[...].astype(F32) * gain[...]
    act = (normed * jax.nn.sigmoid(normed)).astype(BF16)
    for buf, at in zip((own, far, mate, mate_far), quarters(pos, width)):
        part = buf[...]
        mixer[:, pl.ds(at, width)] = part
        total[pl.ds(at, width), :] = dot(part, act, (0, 0))
    if len(outs) == 1:
        outs[0][...] = total[...].astype(BF16)
        return
    for out, masks in zip(outs, SENT):
        rows = out.shape[0] // len(masks)
        for i, mask in enumerate(masks):
            at = pl.multiple_of(jnp.bitwise_xor(pos[1], mask) * rows, rows)
            out[i * rows : (i + 1) * rows, :] = total[pl.ds(at, rows), :].astype(out.dtype)


def project(pos, bufs, norm_hat, norm_gain, parts):
    tokens, width = bufs[0].shape
    model = width * lax.axis_size("tp")
    channels = norm_hat.shape[1]
    outs = [array(model, channels)]
    if parts > 1:
        rows = model // parts
        outs = [array(len(m) * rows, channels, kind=k) for m, k in zip(SENT, (BF16, BF16, F32, F32))]
    return pl.pallas_call(
        project_kernel,
        in_specs=[SMEM] + [VMEM] * 6,
        out_specs=[VMEM] * (1 + len(outs)),
        out_shape=[array(tokens, model)] + outs,
        scratch_shapes=[pltpu.VMEM((model, channels), F32)],
        compiler_params=params(12),
        name="project",
    )(pos, *bufs, norm_hat, norm_gain[None, :])


def added(a, b):
    return a.astype(F32) + b.astype(F32)


def exchanged(block, width):
    count = lax.axis_size("sp")
    shape = block.shape
    block = block.reshape(count, shape[0] // count, width)
    return lax.all_to_all(block, "sp", split_axis=0, concat_axis=0, tiled=True).reshape(shape)


def returned_rows(pos, args, weights):
    moe_input, _, _, _, _ = args
    tok_rows, model_width = moe_input.shape
    sp_count = lax.axis_size("sp")
    capacity = 3 * tok_rows // sp_count
    width = model_width // lax.axis_size("tp")
    ring = sp_count == 8
    parts, wide = (sp_count, WIDE) if ring else (1, 0)
    select, g_own, *slots = dispatch(pos, *args[2:], *args[:2], sp_count, capacity, parts, wide)
    arrived, far, mate, mate_far = {}, {}, {}, {}
    if ring:
        for d, block in zip(PLACES, slots):
            arrived[d] = swapped(block, "sp", d) if d else block
    else:
        arrived[0] = exchanged(slots[0], 2 * width)
    for d, block in arrived.items():
        mate[d] = swapped(block, "tp", 1)
        if d not in PLACES[:wide]:
            far[d] = swapped(block, "tp", 2)
            mate_far[d] = swapped(far[d], "tp", 1)
    flat, plane = [], []

    def experts(group, name):
        rows = arrived[group[0]].shape[0]
        ins, layout = [], []
        for i, d in enumerate(group):
            ins += [arrived[d], mate[d]]
            layout += [(i * rows, 0), (i * rows, 2)]
            if d in far:
                ins += [far[d], mate_far[d]]
                layout += [(i * rows, 1), (i * rows, 3)]
        both, send, keep, *rest = expert_math(
            pos, ins, layout, rows * len(group), *weights, name == "a"
        )
        flat.extend([both] + rest)
        return keep, swapped(send, "tp", 1)

    finals = []
    for name, (direct, routed) in GROUPS.items() if ring else [("c", ((), (0,)))]:
        keep, mates = experts(direct + routed, name)
        rows = keep.shape[0] // len(direct + routed)
        if direct:
            sums = join(keep, mates, rows, len(direct))
            for d, block in zip(direct, sums):
                plane.append(swapped(block, "sp", d) if d else block)
        if routed:
            half, to_far = fold(keep, mates, rows * len(direct))
            to_far = swapped(to_far, "tp", 2)
            sums = join(half, to_far, rows, len(routed))
            for d, block in zip(routed, sums):
                finals.append(swapped(block, "sp", d) if ring else exchanged(block, width))
    others = []
    if plane:
        own, away = early(select, plane)
        others = [own, swapped(away, "tp", 2)]
    grads = weight_math(flat, model_width, weights[0].shape[1])
    return combine(select, g_own, finals, others), grads


def on_device(
    moe_input,
    out_cotangent,
    routes,
    group_weight,
    inner_weight,
    gate_weight,
    up_weight,
    down_weight,
    value_in,
    gate_in,
    conv_taps,
    norm_hat,
    norm_rstd,
    norm_gain,
    out_proj,
):
    tok_rows, model_width = moe_input.shape
    sp_count = lax.axis_size("sp")
    tp_count = lax.axis_size("tp")
    if gate_weight.shape[0] != 1 or tp_count != 4:
        raise ValueError("unsupported mesh")
    pos = jnp.stack([lax.axis_index("tp"), lax.axis_index("sp")]).astype(jnp.int32)
    mixer_part, grads = returned_rows(
        pos,
        (moe_input, out_cotangent, routes, group_weight, inner_weight),
        (gate_weight[0], up_weight[0], down_weight[0]),
    )
    parts = sp_count if sp_count == 8 else 1
    mixer_far = swapped(mixer_part, "tp", 2)
    mixer_mate = swapped(mixer_part, "tp", 1)
    mixer_mate_far = swapped(mixer_far, "tp", 1)
    bufs = (mixer_part, mixer_far, mixer_mate, mixer_mate_far)
    mixer_grad, *blocks = project(pos, bufs, norm_hat, norm_gain, parts)
    if parts > 1:
        away, close, kept_away, kept = blocks
        away = swapped(away, "sp", 1)
        close = swapped(close, "sp", 1)
        far = join(kept_away, away, model_width // parts, 2)
        rows = model_width // parts
        near = added(kept[rows:], close[rows:]).astype(BF16)
        proj_grad = added(kept[:rows], close[:rows])
        for d, block in ((2, near), (4, far[0]), (6, far[1])):
            proj_grad = proj_grad + swapped(block, "sp", d).astype(F32)
    else:
        block = blocks[0].reshape(sp_count, model_width // sp_count, -1)
        block = lax.all_to_all(block, "sp", split_axis=0, concat_axis=0, tiled=True)
        proj_grad = jnp.sum(block.astype(F32), axis=0)
    normed = norm_hat.astype(F32) * norm_gain[None, :]
    norm_sigma = jax.nn.sigmoid(normed)
    silu_grad = jnp.dot(mixer_grad, out_proj, preferred_element_type=F32)
    hat_grad = silu_grad * silu_slope(normed, norm_sigma) * norm_gain[None, :]
    norm_values = norm_hat.astype(F32)
    sums = jnp.stack([jnp.sum(hat_grad, axis=1), jnp.sum(hat_grad * norm_values, axis=1)])
    sums = sums + swapped(sums, "tp", 1)
    grad_sum, grad_dot = sums + swapped(sums, "tp", 2)
    channels = norm_values.shape[1] * tp_count
    conv_grad = norm_rstd[:, None] * (
        hat_grad - grad_sum[:, None] / channels - norm_values * (grad_dot[:, None] / channels)
    )
    tap_count = conv_taps.shape[0]
    incoming = shifted(conv_grad[: tap_count - 1], "sp", -1)
    tap_values = conv_taps.astype(F32)
    short = tap_count - 1
    extended = jnp.concatenate([conv_grad, jnp.zeros_like(incoming)], axis=0)
    glu_grad = jnp.zeros_like(conv_grad)
    for offset in range(tap_count):
        lower = short - offset
        glu_grad = glu_grad + tap_values[offset][None, :] * extended[lower : lower + tok_rows]
    glu_grad = lax.optimization_barrier(glu_grad)
    extended = jnp.concatenate([jnp.zeros_like(incoming), incoming], axis=0)
    edge = jnp.zeros_like(incoming)
    for offset in range(tap_count):
        lower = short - offset
        edge = edge + tap_values[offset][None, :] * extended[lower : lower + short]
    glu_grad = glu_grad + jnp.pad(edge, ((tok_rows - short, 0), (0, 0)))
    input_sigma = jax.nn.sigmoid(gate_in.astype(F32))
    value_grad = (glu_grad * input_sigma).astype(BF16)
    gate_in_grad = (
        glu_grad * value_in.astype(F32) * input_sigma * (1.0 - input_sigma)
    ).astype(BF16)
    return (*(grad[None] for grad in grads), proj_grad, value_grad, gate_in_grad)


def solution(mesh):
    return jax.shard_map(
        on_device,
        mesh=mesh,
        in_specs=(
            P("sp", None),
            P("sp", None),
            P("sp", None),
            P("sp"),
            P("sp", None),
            P("sp", None, "tp"),
            P("sp", None, "tp"),
            P("sp", "tp", None),
            P("sp", "tp"),
            P("sp", "tp"),
            P(None, "tp"),
            P("sp", "tp"),
            P("sp"),
            P("tp"),
            P(None, "tp"),
        ),
        out_specs=(
            P("sp", None, "tp"),
            P("sp", None, "tp"),
            P("sp", "tp", None),
            P("sp", "tp"),
            P("sp", "tp"),
            P("sp", "tp"),
        ),
        check_vma=False,
    )
```

```python
import functools

import jax
import jax.numpy as jnp
from jax import lax
from jax.experimental import pallas as pl
from jax.experimental.pallas import tpu as pltpu
from jax.sharding import PartitionSpec as P


F32 = jnp.float32
BF16 = jnp.bfloat16
VMEM = pl.BlockSpec(memory_space=pltpu.VMEM)
SMEM = pl.BlockSpec(memory_space=pltpu.SMEM)
HBM = pl.BlockSpec(memory_space=pltpu.HBM)


WIDE = 3
GROUPS = {"a": ((0, 1, 2), ()), "b": ((4,), (3, 5)), "c": ((), (6, 7))}
PLACES = sum((g[0] for g in GROUPS.values()), ()) + sum((g[1] for g in GROUPS.values()), ())
SENT = ((5, 7), (1, 3), (4, 6), (0, 2))


def swapped(block, axis, mask):
    count = lax.axis_size(axis)
    return lax.ppermute(block, axis, [(i, i ^ mask) for i in range(count)])


def shifted(block, axis, distance):
    devices = range(lax.axis_size(axis))
    route = [(i - distance, i) for i in devices if i - distance in devices]
    return lax.ppermute(block, axis, route)


def silu_slope(logits, squashed):
    return squashed * (1.0 + logits * (1.0 - squashed))


def dot(a, b, contract):
    return lax.dot_general(a, b, ((contract[:1], contract[1:]), ((), ())), preferred_element_type=F32)


def params(mib):
    return pltpu.CompilerParams(vmem_limit_bytes=mib * 1024 * 1024)


def array(*shape, kind=BF16):
    return jax.ShapeDtypeStruct(shape, kind)


def in_hbm(*arrays):
    return [pltpu.with_memory_space_constraint(a, pltpu.HBM) for a in arrays]


def dispatch_kernel(
    experts, capacity, wide, flip, pos, routes_in, group_in, inner_in, x_all, g_all, select_ref, g_own, *refs
):
    slot_refs, (x_own, x_far, g_far, routes, group, inner, sems) = refs[:-7], refs[-7:]
    tables = [
        pltpu.make_async_copy(source, target, sems.at[4 + i])
        for i, (source, target) in enumerate(
            ((routes_in, routes), (group_in, group), (inner_in, inner))
        )
    ]
    for copy in tables:
        copy.start()
    width = x_own.shape[1]

    def fetch(source, target, quarter, i):
        at = pl.ds(pl.multiple_of(quarter * width, width), width)
        return pltpu.make_async_copy(source.at[:, at], target, sems.at[i])

    far = jnp.bitwise_xor(pos[0], 2)
    copies = [fetch(x_all, x_own, pos[0], 0), fetch(g_all, g_own, pos[0], 1)]
    if wide:
        copies += [fetch(x_all, x_far, far, 2), fetch(g_all, g_far, far, 3)]
    for copy in copies:
        copy.start()
    for copy in tables:
        copy.wait()
    tokens = routes.shape[1]
    slots = experts * capacity
    expert = lax.broadcasted_iota(jnp.int32, (experts, tokens), 0)
    earlier = lax.broadcasted_iota(jnp.int32, (tokens, tokens), 0)
    later = lax.broadcasted_iota(jnp.int32, (tokens, tokens), 1)
    before = (earlier < later).astype(F32).astype(BF16)
    slot_number = lax.broadcasted_iota(jnp.int32, (slots, tokens), 0)
    base = jnp.zeros((experts, 1), F32)
    select = jnp.zeros((slots, tokens), F32)
    weight = jnp.zeros((slots, tokens), F32)
    for k in range(2):
        route = routes[k : k + 1, :]
        hot = (expert == route).astype(F32)
        counts = dot(hot.astype(BF16), before, (1, 0)) + base
        base = base + jnp.sum(hot, axis=1, keepdims=True)
        rank = jnp.sum(hot * counts, axis=0, keepdims=True).astype(jnp.int32)
        owner = route
        if flip:
            mask = jnp.bitwise_xor(route, pos[1])
            owner = mask
            for place, own in enumerate(PLACES):
                if place != own:
                    owner = jnp.where(mask == own, place, owner)
        hit = slot_number == owner * capacity + rank
        select = jnp.where(hit, 1.0, select)
        weight = jnp.where(hit, group[...] * inner[k : k + 1, :], weight)
    select = select.astype(BF16)
    select_ref[...] = select
    weight = jnp.sum(weight, axis=1, keepdims=True)
    rows = slots // len(slot_refs)
    for copy in copies:
        copy.wait()
    picked_x = dot(select, x_own[...], (1, 0)).astype(BF16)
    picked_g = (weight * dot(select, g_own[...], (1, 0))).astype(BF16)
    for i, out in enumerate(slot_refs):
        out[:, :width] = picked_x[i * rows : (i + 1) * rows]
        out[:, width : 2 * width] = picked_g[i * rows : (i + 1) * rows]
    if wide:
        select, weight = select[: wide * rows], weight[: wide * rows]
        picked_x = dot(select, x_far[...], (1, 0)).astype(BF16)
        picked_g = (weight * dot(select, g_far[...], (1, 0))).astype(BF16)
        for i, out in enumerate(slot_refs[:wide]):
            out[:, 2 * width : 3 * width] = picked_x[i * rows : (i + 1) * rows]
            out[:, 3 * width :] = picked_g[i * rows : (i + 1) * rows]


def dispatch(pos, routes, group_weight, inner_weight, x, g, experts, capacity, parts, wide):
    tokens, model = x.shape
    width = model // lax.axis_size("tp")
    slots = experts * capacity
    rows = slots // parts
    return pl.pallas_call(
        functools.partial(dispatch_kernel, experts, capacity, wide, parts > 1),
        in_specs=[SMEM] + [HBM] * 5,
        out_specs=[VMEM] * (2 + parts),
        out_shape=[array(slots, tokens), array(tokens, width)]
        + [array(rows, (4 if i < wide else 2) * width) for i in range(parts)],
        scratch_shapes=[pltpu.VMEM((tokens, width), BF16)] * 3
        + [
            pltpu.VMEM((2, tokens), jnp.int32),
            pltpu.VMEM((1, tokens), F32),
            pltpu.VMEM((2, tokens), F32),
            pltpu.SemaphoreType.DMA((7,)),
        ],
        compiler_params=params(20),
        name="dispatch",
    )(pos, *in_hbm(routes.T, group_weight[None, :], inner_weight.T, x, g))


def quarters(pos, width):
    p = pos[0]
    order = [p, jnp.bitwise_xor(p, 2), jnp.bitwise_xor(p, 1), jnp.bitwise_xor(p, 3)]
    return [pl.multiple_of(q * width, width) for q in order]


def expert_kernel(layout, fetch, pos, *refs):
    if fetch:
        refs, (fetched, sem) = refs[:-2], refs[-2:]
    ins, (wg, wu, wd, both, send, keep, gd, ud, ha) = refs[:-9], refs[-9:]
    if fetch:
        copy = pltpu.make_async_copy(wd, fetched, sem)
        copy.start()
    width = keep.shape[1] // 2
    model = both.shape[1] // 2
    order = quarters(pos, width)
    for ref, (row, which) in zip(ins, layout):
        rows = slice(row, row + ref.shape[0])
        for i in range(ref.shape[1] // (2 * width)):
            at = order[which + i]
            lower = 2 * i * width
            both[rows, pl.ds(at, width)] = ref[:, lower : lower + width]
            at = pl.multiple_of(model + at, width)
            both[rows, pl.ds(at, width)] = ref[:, lower + width : lower + 2 * width]
    gate = dot(both[:, :model], wg[...], (1, 0))
    up = dot(both[:, :model], wu[...], (1, 0))
    if fetch:
        copy.wait()
        wd = fetched
    act = dot(both[:, model:], wd[...], (1, 1))
    sigma = jax.nn.sigmoid(gate)
    ha[...] = (gate * sigma * up).astype(BF16)
    gate_delta = (act * up * silu_slope(gate, sigma)).astype(BF16)
    up_delta = (act * gate * sigma).astype(BF16)
    gd[...] = gate_delta
    ud[...] = up_delta

    def partial_of(at):
        value = dot(gate_delta, wg[pl.ds(at, width), :], (1, 1))
        value = value + dot(up_delta, wu[pl.ds(at, width), :], (1, 1))
        return value.astype(BF16)

    send[:, :width] = partial_of(order[2])
    send[:, width:] = partial_of(order[3])
    keep[:, :width] = partial_of(order[0])
    keep[:, width:] = partial_of(order[1])


def expert_math(pos, blocks, layout, rows, wg, wu, wd, fetch):
    model, hidden = wg.shape
    width = model // lax.axis_size("tp")
    return pl.pallas_call(
        functools.partial(expert_kernel, layout, fetch),
        in_specs=[SMEM] + [VMEM] * (len(blocks) + 2) + [HBM if fetch else VMEM],
        out_specs=[VMEM] * 6,
        out_shape=[array(rows, 2 * model)]
        + [array(rows, 2 * width)] * 2
        + [array(rows, hidden)] * 3,
        scratch_shapes=[pltpu.VMEM(wd.shape, BF16), pltpu.SemaphoreType.DMA] if fetch else [],
        compiler_params=params(20),
        name="expert",
    )(pos, *blocks, wg, wu, *(in_hbm(wd) if fetch else [wd]))


def gates_kernel(groups, *refs):
    ins, (gate_grad, up_grad) = refs[: 3 * groups], refs[3 * groups :]
    model, hidden = gate_grad.shape
    width = model // 4
    for at in range(0, model, width):
        gate = jnp.zeros((width, hidden), F32)
        up = jnp.zeros((width, hidden), F32)
        for i in range(groups):
            both, gd, ud = ins[3 * i : 3 * i + 3]
            part = both[:, at : at + width]
            gate = gate + dot(part, gd[...], (0, 0))
            up = up + dot(part, ud[...], (0, 0))
        gate_grad[at : at + width, :] = gate.astype(BF16)
        up_grad[at : at + width, :] = up.astype(BF16)


def downs_kernel(groups, *refs):
    ins, down_grad = refs[: 2 * groups], refs[2 * groups]
    hidden, model = down_grad.shape
    width = model // 4
    for at in range(0, model, width):
        down = jnp.zeros((hidden, width), F32)
        for i in range(groups):
            both, ha = ins[2 * i : 2 * i + 2]
            down = down + dot(ha[...], both[:, model + at : model + at + width], (0, 0))
        down_grad[:, at : at + width] = down.astype(BF16)


def weight_math(flat, model, hidden):
    groups = [flat[i : i + 4] for i in range(0, len(flat), 4)]
    gates_in = [a for both, gd, ud, ha in groups for a in (both, gd, ud)]
    downs_in = [a for both, gd, ud, ha in groups for a in (both, ha)]
    gate_grad, up_grad = pl.pallas_call(
        functools.partial(gates_kernel, len(groups)),
        in_specs=[VMEM] * len(gates_in),
        out_specs=[VMEM] * 2,
        out_shape=[array(model, hidden)] * 2,
        compiler_params=params(20),
        name="gates",
    )(*gates_in)
    down_grad = pl.pallas_call(
        functools.partial(downs_kernel, len(groups)),
        in_specs=[VMEM] * len(downs_in),
        out_specs=VMEM,
        out_shape=array(hidden, model),
        compiler_params=params(20),
        name="downs",
    )(*downs_in)
    return gate_grad, up_grad, down_grad


def join_kernel(keep, mate, *outs):
    row = 0
    for out in outs:
        rows = slice(row, row + out.shape[0])
        out[...] = (keep[rows, :].astype(F32) + mate[rows, :].astype(F32)).astype(BF16)
        row += out.shape[0]


def join(keep, mate, rows, parts):
    return pl.pallas_call(
        join_kernel,
        in_specs=[VMEM] * 2,
        out_specs=[VMEM] * parts,
        out_shape=[array(rows, keep.shape[1])] * parts,
        compiler_params=params(12),
        name="join",
    )(keep, mate)


def fold_kernel(start, keep, mate, half, far):
    width = half.shape[1]
    half[...] = keep[start:, :width].astype(F32) + mate[start:, :width].astype(F32)
    far[...] = (keep[start:, width:].astype(F32) + mate[start:, width:].astype(F32)).astype(BF16)


def fold(keep, mate, start):
    rows, double = keep.shape
    shape = (rows - start, double // 2)
    return pl.pallas_call(
        functools.partial(fold_kernel, start),
        in_specs=[VMEM] * 2,
        out_specs=[VMEM] * 2,
        out_shape=[array(*shape, kind=F32), array(*shape)],
        compiler_params=params(12),
        name="fold",
    )(keep, mate)


def stacked(blocks, rows):
    at = 0
    for block in blocks:
        rows[at : at + block.shape[0], :] = block[...]
        at += block.shape[0]


def early_kernel(select, *refs):
    blocks, (keep, far, rows) = refs[:-3], refs[-3:]
    stacked(blocks, rows)
    width = keep.shape[1]
    total = dot(select[: rows.shape[0], :], rows[...], (0, 0))
    keep[...] = total[:, :width]
    far[...] = total[:, width:].astype(BF16)


def early(select, blocks):
    tokens = select.shape[1]
    rows = sum(b.shape[0] for b in blocks)
    width = blocks[0].shape[1] // 2
    return pl.pallas_call(
        early_kernel,
        in_specs=[VMEM] * (1 + len(blocks)),
        out_specs=[VMEM] * 2,
        out_shape=[array(tokens, width, kind=F32), array(tokens, width)],
        scratch_shapes=[pltpu.VMEM((rows, 2 * width), BF16)],
        compiler_params=params(12),
        name="early",
    )(select, *blocks)


def combine_kernel(count, select, g_own, *refs):
    blocks, others, (out, rows) = refs[:count], refs[count:-2], refs[-2:]
    stacked(blocks, rows)
    total = dot(select[select.shape[0] - rows.shape[0] :, :], rows[...], (0, 0))
    for other in others:
        total = total + other[...].astype(F32)
    out[...] = (g_own[...].astype(F32) + total).astype(BF16)


def combine(select, g, blocks, others):
    tokens = select.shape[1]
    width = blocks[0].shape[1]
    rows = sum(b.shape[0] for b in blocks)
    return pl.pallas_call(
        functools.partial(combine_kernel, len(blocks)),
        in_specs=[VMEM] * (2 + len(blocks) + len(others)),
        out_specs=VMEM,
        out_shape=array(tokens, width),
        scratch_shapes=[pltpu.VMEM((rows, width), BF16)],
        compiler_params=params(12),
        name="combine",
    )(select, g, *blocks, *others)


def project_kernel(pos, own, far, mate, mate_far, hat, gain, mixer, *refs):
    outs, total = refs[:-1], refs[-1]
    width = own.shape[1]
    normed = hat[...].astype(F32) * gain[...]
    act = (normed * jax.nn.sigmoid(normed)).astype(BF16)
    for buf, at in zip((own, far, mate, mate_far), quarters(pos, width)):
        part = buf[...]
        mixer[:, pl.ds(at, width)] = part
        total[pl.ds(at, width), :] = dot(part, act, (0, 0))
    if len(outs) == 1:
        outs[0][...] = total[...].astype(BF16)
        return
    for out, masks in zip(outs, SENT):
        rows = out.shape[0] // len(masks)
        for i, mask in enumerate(masks):
            at = pl.multiple_of(jnp.bitwise_xor(pos[1], mask) * rows, rows)
            out[i * rows : (i + 1) * rows, :] = total[pl.ds(at, rows), :].astype(out.dtype)


def project(pos, bufs, norm_hat, norm_gain, parts):
    tokens, width = bufs[0].shape
    model = width * lax.axis_size("tp")
    channels = norm_hat.shape[1]
    outs = [array(model, channels)]
    if parts > 1:
        rows = model // parts
        outs = [array(len(m) * rows, channels, kind=k) for m, k in zip(SENT, (BF16, BF16, F32, F32))]
    return pl.pallas_call(
        project_kernel,
        in_specs=[SMEM] + [VMEM] * 6,
        out_specs=[VMEM] * (1 + len(outs)),
        out_shape=[array(tokens, model)] + outs,
        scratch_shapes=[pltpu.VMEM((model, channels), F32)],
        compiler_params=params(12),
        name="project",
    )(pos, *bufs, norm_hat, norm_gain[None, :])


def added(a, b):
    return a.astype(F32) + b.astype(F32)


def exchanged(block, width):
    count = lax.axis_size("sp")
    shape = block.shape
    block = block.reshape(count, shape[0] // count, width)
    return lax.all_to_all(block, "sp", split_axis=0, concat_axis=0, tiled=True).reshape(shape)


def returned_rows(pos, args, weights):
    moe_input, _, _, _, _ = args
    tok_rows, model_width = moe_input.shape
    sp_count = lax.axis_size("sp")
    capacity = 3 * tok_rows // sp_count
    width = model_width // lax.axis_size("tp")
    ring = sp_count == 8
    parts, wide = (sp_count, WIDE) if ring else (1, 0)
    select, g_own, *slots = dispatch(pos, *args[2:], *args[:2], sp_count, capacity, parts, wide)
    arrived, far, mate, mate_far = {}, {}, {}, {}
    if ring:
        for d, block in zip(PLACES, slots):
            arrived[d] = swapped(block, "sp", d) if d else block
    else:
        arrived[0] = exchanged(slots[0], 2 * width)
    for d, block in arrived.items():
        mate[d] = swapped(block, "tp", 1)
        if d not in PLACES[:wide]:
            far[d] = swapped(block, "tp", 2)
            mate_far[d] = swapped(far[d], "tp", 1)
    flat, plane = [], []

    def experts(group, name):
        rows = arrived[group[0]].shape[0]
        ins, layout = [], []
        for i, d in enumerate(group):
            ins += [arrived[d], mate[d]]
            layout += [(i * rows, 0), (i * rows, 2)]
            if d in far:
                ins += [far[d], mate_far[d]]
                layout += [(i * rows, 1), (i * rows, 3)]
        both, send, keep, *rest = expert_math(
            pos, ins, layout, rows * len(group), *weights, name == "a"
        )
        flat.extend([both] + rest)
        return keep, swapped(send, "tp", 1)

    finals = []
    for name, (direct, routed) in GROUPS.items() if ring else [("c", ((), (0,)))]:
        keep, mates = experts(direct + routed, name)
        rows = keep.shape[0] // len(direct + routed)
        if direct:
            sums = join(keep, mates, rows, len(direct))
            for d, block in zip(direct, sums):
                plane.append(swapped(block, "sp", d) if d else block)
        if routed:
            half, to_far = fold(keep, mates, rows * len(direct))
            to_far = swapped(to_far, "tp", 2)
            sums = join(half, to_far, rows, len(routed))
            for d, block in zip(routed, sums):
                finals.append(swapped(block, "sp", d) if ring else exchanged(block, width))
    others = []
    if plane:
        own, away = early(select, plane)
        others = [own, swapped(away, "tp", 2)]
    grads = weight_math(flat, model_width, weights[0].shape[1])
    return combine(select, g_own, finals, others), grads


def on_device(
    moe_input,
    out_cotangent,
    routes,
    group_weight,
    inner_weight,
    gate_weight,
    up_weight,
    down_weight,
    value_in,
    gate_in,
    conv_taps,
    norm_hat,
    norm_rstd,
    norm_gain,
    out_proj,
):
    tok_rows, model_width = moe_input.shape
    sp_count = lax.axis_size("sp")
    tp_count = lax.axis_size("tp")
    if gate_weight.shape[0] != 1 or tp_count != 4:
        raise ValueError("unsupported mesh")
    pos = jnp.stack([lax.axis_index("tp"), lax.axis_index("sp")]).astype(jnp.int32)
    mixer_part, grads = returned_rows(
        pos,
        (moe_input, out_cotangent, routes, group_weight, inner_weight),
        (gate_weight[0], up_weight[0], down_weight[0]),
    )
    parts = sp_count if sp_count == 8 else 1
    mixer_far = swapped(mixer_part, "tp", 2)
    mixer_mate = swapped(mixer_part, "tp", 1)
    mixer_mate_far = swapped(mixer_far, "tp", 1)
    bufs = (mixer_part, mixer_far, mixer_mate, mixer_mate_far)
    mixer_grad, *blocks = project(pos, bufs, norm_hat, norm_gain, parts)
    if parts > 1:
        away, close, kept_away, kept = blocks
        away = swapped(away, "sp", 1)
        close = swapped(close, "sp", 1)
        far = join(kept_away, away, model_width // parts, 2)
        rows = model_width // parts
        near = added(kept[rows:], close[rows:]).astype(BF16)
        proj_grad = added(kept[:rows], close[:rows])
        for d, block in ((2, near), (4, far[0]), (6, far[1])):
            proj_grad = proj_grad + swapped(block, "sp", d).astype(F32)
    else:
        block = blocks[0].reshape(sp_count, model_width // sp_count, -1)
        block = lax.all_to_all(block, "sp", split_axis=0, concat_axis=0, tiled=True)
        proj_grad = jnp.sum(block.astype(F32), axis=0)
    normed = norm_hat.astype(F32) * norm_gain[None, :]
    norm_sigma = jax.nn.sigmoid(normed)
    silu_grad = jnp.dot(mixer_grad, out_proj, preferred_element_type=F32)
    hat_grad = silu_grad * silu_slope(normed, norm_sigma) * norm_gain[None, :]
    norm_values = norm_hat.astype(F32)
    sums = jnp.stack([jnp.sum(hat_grad, axis=1), jnp.sum(hat_grad * norm_values, axis=1)])
    sums = sums + swapped(sums, "tp", 1)
    grad_sum, grad_dot = sums + swapped(sums, "tp", 2)
    channels = norm_values.shape[1] * tp_count
    conv_grad = norm_rstd[:, None] * (
        hat_grad - grad_sum[:, None] / channels - norm_values * (grad_dot[:, None] / channels)
    )
    tap_count = conv_taps.shape[0]
    incoming = shifted(conv_grad[: tap_count - 1], "sp", -1)
    tap_values = conv_taps.astype(F32)
    short = tap_count - 1
    extended = jnp.concatenate([conv_grad, jnp.zeros_like(incoming)], axis=0)
    glu_grad = jnp.zeros_like(conv_grad)
    for offset in range(tap_count):
        lower = short - offset
        glu_grad = glu_grad + tap_values[offset][None, :] * extended[lower : lower + tok_rows]
    glu_grad = lax.optimization_barrier(glu_grad)
    extended = jnp.concatenate([jnp.zeros_like(incoming), incoming], axis=0)
    edge = jnp.zeros_like(incoming)
    for offset in range(tap_count):
        lower = short - offset
        edge = edge + tap_values[offset][None, :] * extended[lower : lower + short]
    glu_grad = glu_grad + jnp.pad(edge, ((tok_rows - short, 0), (0, 0)))
    input_sigma = jax.nn.sigmoid(gate_in.astype(F32))
    value_grad = (glu_grad * input_sigma).astype(BF16)
    gate_in_grad = (
        glu_grad * value_in.astype(F32) * input_sigma * (1.0 - input_sigma)
    ).astype(BF16)
    return (*(grad[None] for grad in grads), proj_grad, value_grad, gate_in_grad)


def solution(mesh):
    return jax.shard_map(
        on_device,
        mesh=mesh,
        in_specs=(
            P("sp", None),
            P("sp", None),
            P("sp", None),
            P("sp"),
            P("sp", None),
            P("sp", None, "tp"),
            P("sp", None, "tp"),
            P("sp", "tp", None),
            P("sp", "tp"),
            P("sp", "tp"),
            P(None, "tp"),
            P("sp", "tp"),
            P("sp"),
            P("tp"),
            P(None, "tp"),
        ),
        out_specs=(
            P("sp", None, "tp"),
            P("sp", None, "tp"),
            P("sp", "tp", None),
            P("sp", "tp"),
            P("sp", "tp"),
            P("sp", "tp"),
        ),
        check_vma=False,
    )
```
